32 devices in a mesh: fs: 16 (over z, y, x), tp: 2 (over core).
Axes of the slice: x: 2, y: 2, z: 4, core: 2. Of those that a mesh axis runs over, the one named last changes fastest.
Arguments:
- tokens: bfloat16 [12288, 2048], P('fs'), may hold values from -6 to 6
- norm_gain: float32 [2048], replicated, may hold values from 0.1 to 1.9
- up_weight: float32 [2048, 8192], P('fs', 'tp'), may hold values from -0.125 to 0.125
- up_scale: float32 [8192], P('tp'), may hold values from 0.5 to 2
- down_weight: float32 [8192, 2048], P('tp', 'fs'), may hold values from -0.09375 to 0.09375
- down_scale: float32 [1, 2048], replicated, may hold values from 0.5 to 2
Outputs:
- mixed: bfloat16 [12288, 2048], P('fs', 'tp')
The draws below stay inside these ranges and needn't reach their ends.
All inputs are finite; a program needn't handle non-finite values.
Results may differ from the reference program's by a relative error of at most 0.014.
Values may be sent and summed in bfloat16 or wider, within the bound.
A program may use at most 128 MiB of HBM per device.

```python
import math
import jax
import jax.numpy as jnp
from jax import lax

D = 2048
FF = 8192
TOKENS = 12288
N_FS = 16
N_TP = 2


def with_spikes(drawn, stream_key, source, target, shards_of, factor):
    def block_of(axis_at):
        return (jnp.arange(drawn.shape[axis_at]) // (drawn.shape[axis_at] // shards_of)).reshape((-1,) + (1,) * (drawn.ndim - 1 - axis_at))

    near = jax.random.permutation(stream_key, shards_of)[block_of(target)]
    far = (block_of(target) + shards_of // 2) % shards_of
    return jnp.where((block_of(source) == near) | (block_of(source) == far), factor * drawn, drawn)


def level_of(key, extent, cuts, low, high):
    level = 1.0
    for dim, shards_of in cuts:
        draws = jax.random.uniform(jax.random.fold_in(jax.random.fold_in(key, 6), dim), (shards_of,), jnp.float32, low / len(cuts), high / len(cuts))
        level = level * jnp.repeat(jnp.exp(draws), extent[dim] // shards_of).reshape((-1,) + (1,) * (len(extent) - 1 - dim))
    return level


def bell_draw(stream_key, extent, deviation, bound, shards=(), dtype=jnp.bfloat16):
    factor_of = level_of(stream_key, extent, shards, -0.22, 0.18) if shards else 1.0
    drawn = jax.random.normal(stream_key, extent, jnp.float32) * deviation * factor_of
    return jnp.minimum(jnp.maximum(drawn, -bound), bound).astype(dtype)


def gaussian_with(key, shape, spread, most, pieces, heavy, held_as=jnp.bfloat16):
    drawn = spread * jax.random.normal(key, shape, jnp.float32)
    if pieces:
        drawn = drawn * level_of(key, shape, pieces, -0.22, 0.18)
    return jnp.clip(with_spikes(drawn, jax.random.fold_in(key, 3), *heavy), -most, most).astype(held_as)


def setup_inputs(seed: int = 0) -> dict:
    arg_keys = jax.random.split(jax.random.key(seed), 7)
    tokens = bell_draw(arg_keys[0], (TOKENS, D), 1.0, 6.0, ((0, 16),))
    norm_gain = jnp.clip(1.0 + 0.18 * jax.random.normal(arg_keys[1], (D,), jnp.float32), 0.1, 1.9)
    up_weight = bell_draw(arg_keys[2], (D, FF), D ** -0.5, 0.125, ((0, 16), (1, 2)), jnp.float32)
    up_scale = jnp.clip(jnp.exp(math.log(2.0) - 1.3862944 * jax.random.uniform(arg_keys[3], (FF,), jnp.float32) ** level_of(arg_keys[3], (FF,), ((0, 2),), -0.2, 0.2)), 0.5, 2.0)
    down_weight = gaussian_with(arg_keys[4], (FF, D), FF ** -0.5, 0.09375, ((0, 2), (1, 16)), (0, 1, 16, 2.0), jnp.float32)
    down_scale = jnp.clip(jnp.exp(jax.random.uniform(arg_keys[5], (1, D), jnp.float32, math.log(0.5), math.log(2.0))), 0.5, 2.0)
    return dict(tokens=tokens, norm_gain=norm_gain, up_weight=up_weight, up_scale=up_scale, down_weight=down_weight, down_scale=down_scale)


def reference(tokens, norm_gain, up_weight, up_scale, down_weight, down_scale):
    up_cast = up_weight.astype(jnp.bfloat16)
    down_cast = down_weight.astype(jnp.bfloat16)
    block_ff = FF // N_TP
    groups = tokens.reshape(N_FS, TOKENS // N_FS, D)

    def one_group(rows):
        values = rows.astype(jnp.float32)
        normed = (values * lax.rsqrt(lax.optimization_barrier(jnp.mean(values * values, axis=-1, keepdims=True)) + 1e-06) * norm_gain).astype(jnp.bfloat16)
        pre = jnp.dot(normed, up_cast, preferred_element_type=jnp.float32) * up_scale
        hidden = jnp.square(jnp.maximum(pre, 0.0)).astype(jnp.bfloat16)
        total = jnp.zeros((rows.shape[0], D), jnp.float32)
        for block in range(N_TP):
            lower = block * block_ff
            partial_value = jnp.dot(hidden[:, lower:lower + block_ff], down_cast[lower:lower + block_ff, :], preferred_element_type=jnp.float32) * down_scale
            total = total + partial_value.astype(jnp.bfloat16).astype(jnp.float32)
        return total.astype(jnp.bfloat16)
    return lax.map(one_group, groups).reshape(TOKENS, D)
```

```python
import functools

import jax
import jax.numpy as jnp
from jax import lax
from jax.experimental import pallas as pl
from jax.experimental.pallas import tpu as pltpu
from jax.sharding import PartitionSpec as P

MESH = pl.DeviceIdType.MESH
SIDE = 2
GROUP = SIDE * SIDE
CORES = 2
COLS = 256


def gathered(tokens, norm_gain, up_weight, up_scale, down_weight, down_scale):
    values = tokens.astype(jnp.float32)
    normed = (
        values * lax.rsqrt(jnp.mean(values * values, axis=-1, keepdims=True) + 1e-06) * norm_gain
    ).astype(jnp.bfloat16)
    up_cast = up_weight.astype(jnp.bfloat16)
    down_cast = down_weight.astype(jnp.bfloat16)
    up_full = lax.all_gather(up_cast, "fs", axis=0, tiled=True)
    pre = jnp.dot(normed, up_full, preferred_element_type=jnp.float32) * up_scale
    hidden = jnp.square(jnp.maximum(pre, 0.0)).astype(jnp.bfloat16)
    down_full = lax.all_gather(down_cast, "fs", axis=1, tiled=True)
    partial_value = jnp.dot(hidden, down_full, preferred_element_type=jnp.float32) * down_scale
    rounded = partial_value.astype(jnp.bfloat16)
    return (
        lax.psum_scatter(rounded, "tp", scatter_dimension=1, tiled=True)
        .astype(jnp.float32)
        .astype(jnp.bfloat16)
    )


def layer_kernel(
    layers, rows, normed, up_in, down_in, up_scale, down_scale, out,
    tok, upb, downb, hid, stage, partner, summed, peers, own,
    local_sem, piece_recv, piece_send, level_send, tok_recv, tok_send,
    mate_recv, mate_send, part_recv, part_send, red_recv, red_send,
):
    fs = lax.axis_index("fs")
    core = lax.axis_index("tp")
    z, q = fs // GROUP, fs % GROUP
    depth, width = up_in.shape[0], upb.shape[1]
    half = rows // CORES
    sub = half // 2
    units = 2 * layers
    per_layer = GROUP * depth // COLS
    per_unit = COLS // depth

    def at(r):
        return ((q // SIDE + r // SIDE) % SIDE) * SIDE + (q % SIDE + r % SIDE) % SIDE

    def chip(layer, inner):
        return (layer * GROUP + inner, core)

    mate = (fs, 1 - core)

    barrier = pltpu.get_barrier_semaphore()
    for r in range(1, GROUP):
        pl.semaphore_signal(barrier, inc=1, device_id=chip(z, at(r)), device_id_type=MESH)
    pl.semaphore_signal(barrier, inc=1, device_id=mate, device_id_type=MESH)

    @pl.when(z > 0)
    def _():
        pl.semaphore_signal(barrier, inc=1, device_id=chip(z - 1, q), device_id_type=MESH)

    @pl.when(z < layers - 1)
    def _():
        pl.semaphore_signal(barrier, inc=1, device_id=chip(z + 1, q), device_id_type=MESH)

    def slot(kind, layer, inner):
        if kind == 0:
            return upb.at[pl.ds(pl.multiple_of((layer * GROUP + inner) * depth, depth), depth), :]
        return downb.at[layer, :, pl.ds(pl.multiple_of(inner * depth, depth), depth)]

    def source(kind, inner):
        if kind == 0:
            return up_in.at[:, pl.ds(pl.multiple_of(inner * width, width), width)]
        return down_in.at[pl.ds(pl.multiple_of(inner * width, width), width), :]

    def remote(src, dst, send, recv, device):
        return pltpu.make_async_remote_copy(
            src_ref=src, dst_ref=dst, send_sem=send, recv_sem=recv,
            device_id=device, device_id_type=MESH,
        )

    def along(kind, layer, inner, way):
        piece = slot(kind, layer, inner)
        index = layer * GROUP + inner
        return remote(
            piece, piece, piece_send.at[kind, index, way], piece_recv.at[kind, index],
            chip(z + 2 * way - 1, q),
        )

    def level(kind, r):
        return remote(
            source(kind, at(r)), slot(kind, z, q), level_send.at[kind, r - 1],
            piece_recv.at[kind, fs], chip(z, at(r)),
        )

    def each_way(kind, layer, inner, act):
        @pl.when(jnp.logical_and(layer <= z, z < layers - 1))
        def _():
            act(along(kind, layer, inner, 1))

        @pl.when(jnp.logical_and(layer >= z, z > 0))
        def _():
            act(along(kind, layer, inner, 0))

    def start(copy):
        copy.start()

    def finish_send(copy):
        copy.wait_send()

    def arrived(kind, layer, inner):
        piece = slot(kind, layer, inner)
        remote(
            piece, piece, piece_send.at[kind, layer * GROUP + inner, 0],
            piece_recv.at[kind, layer * GROUP + inner], mate,
        ).wait_recv()

    def block(inner, side, s):
        return tok.at[pl.ds(pl.multiple_of(inner * rows + side * half + s * sub, sub), sub), :]

    def hand(r, s):
        return remote(
            normed.at[pl.ds(pl.multiple_of(core * half + s * sub, sub), sub), :],
            block(q, core, s), tok_send.at[r - 1, s], tok_recv.at[r - 1, s], chip(z, at(r)),
        )

    def pass_on(came, to, s):
        piece = block(at(came), core, s)
        return remote(
            piece, piece, tok_send.at[GROUP - 2, s], tok_recv.at[GROUP - 2, s], chip(z, at(to))
        )

    def tok_arrived(r, s):
        piece = block(at(r), core, s)
        remote(piece, piece, tok_send.at[r - 1, s], tok_recv.at[r - 1, s], mate).wait_recv()

    def share(r, s):
        piece = block(at(r), core, s)
        return remote(piece, piece, mate_send.at[r - 1, s], mate_recv.at[r - 1, s], mate)

    locals_ = [
        pltpu.make_async_copy(source(0, q), slot(0, z, q), local_sem.at[0]),
        pltpu.make_async_copy(source(1, q), slot(1, z, q), local_sem.at[1]),
        pltpu.make_async_copy(
            normed, tok.at[pl.ds(pl.multiple_of(q * rows, rows), rows), :], local_sem.at[2]
        ),
    ]
    for copy in locals_:
        copy.start()
    greeted = GROUP + jnp.where(z > 0, 1, 0) + jnp.where(z < layers - 1, 1, 0)
    pl.semaphore_wait(barrier, greeted)

    for r in (3, 1, 2):
        level(0, r).start()
    hand(1, 0).start()
    hand(2, 1).start()
    hand(1, 1).start()
    hand(2, 0).start()
    for r in (3, 1, 2):
        level(1, r).start()
    for copy in locals_:
        copy.wait()
    each_way(0, z, q, start)
    for r in (1, 2, 3):
        arrived(0, z, at(r))
        each_way(0, z, at(r), start)

    def from_afar(d):
        for r in range(GROUP):
            @pl.when(z - d >= 0)
            def _():
                arrived(0, z - d, at(r))
                each_way(0, z - d, at(r), start)

            @pl.when(z + d < layers)
            def _():
                arrived(0, z + d, at(r))
                each_way(0, z + d, at(r), start)

    for d in range(1, layers):
        from_afar(d)
        if d == 1:
            tok_arrived(1, 0)
            pass_on(1, 2, 0).start()
            share(1, 0).start()
            tok_arrived(2, 1)
            pass_on(2, 1, 1).start()
            share(2, 1).start()

    each_way(1, z, q, start)
    for r in (1, 2, 3):
        arrived(1, z, at(r))
        each_way(1, z, at(r), start)
    for r, s in ((1, 1), (2, 0), (3, 0), (3, 1)):
        tok_arrived(r, s)
        share(r, s).start()
    for r in (1, 2, 3):
        for s in (0, 1):
            piece = block(at(r), 1 - core, s)
            remote(piece, piece, mate_send.at[r - 1, s], mate_recv.at[r - 1, s], mate).wait_recv()

    tall = rows * 2 // 3
    wide = 256
    across = width // wide

    def first(i, carry):
        m = pl.ds(pl.multiple_of((i // across) * tall, tall), tall)
        at_n = pl.multiple_of((i % across) * wide, wide)
        pre = jnp.dot(tok[m, :], upb[:, pl.ds(at_n, wide)], preferred_element_type=jnp.float32)
        pre = pre * up_scale[:, pl.ds(pl.multiple_of(q * width + at_n, wide), wide)]
        hid[m, pl.ds(at_n, wide)] = jnp.square(jnp.maximum(pre, 0.0)).astype(hid.dtype)
        return carry

    lax.fori_loop(0, (GROUP * rows // tall) * across, first, 0)

    def red(u, r):
        return remote(
            summed.at[u, at(r)], peers.at[u, r - 1], red_send.at[u, r - 1],
            red_recv.at[u, r - 1], chip(z, at(r)),
        )

    def part(u, b):
        return remote(
            stage.at[u, b], partner.at[u, b], part_send.at[u, b], part_recv.at[u, b], mate
        )

    def second(t, carry):
        s, h = t // per_layer, t % per_layer
        low = 2 * z < layers
        layer = jnp.where(
            low,
            jnp.where(s <= z, z - s, s),
            jnp.where(s <= layers - 1 - z, z + s, layers - 1 - s),
        )

        @pl.when(s > 0)
        def _():
            for k in range(per_unit):
                arrived(1, layer, h * per_unit + k)
                each_way(1, layer, h * per_unit + k, start)

        unit = layer * per_layer + h
        owner = unit // (units // CORES)
        u = unit % (units // CORES)
        cols = pl.ds(pl.multiple_of(h * COLS, COLS), COLS)
        scale = pl.ds(pl.multiple_of(unit * COLS, COLS), COLS)

        def product(b):
            m = pl.ds(pl.multiple_of(b * rows, rows), rows)
            value = jnp.dot(hid[m, :], downb[layer, :, cols], preferred_element_type=jnp.float32)
            return value * down_scale[:, scale]

        @pl.when(owner != core)
        def _():
            def away(i, c):
                b = at(GROUP - 1 - i)
                stage[u, b] = product(b).astype(stage.dtype)
                part(u, b).start()
                return c

            lax.fori_loop(0, GROUP, away, 0)

        @pl.when(owner == core)
        def _():
            def mine(i, c):
                own[at(GROUP - 1 - i)] = product(at(GROUP - 1 - i))
                return c

            lax.fori_loop(0, GROUP, mine, 0)
            for r in (3, 2, 1, 0):
                b = at(r)
                part(u, b).wait_recv()
                summed[u, b] = (own[b] + partner[u, b].astype(jnp.float32)).astype(summed.dtype)
                if r:
                    red(u, r).start()

        return carry

    lax.fori_loop(0, units, second, 0)

    def last(u, carry):
        for r in range(1, GROUP):
            red(u, r).wait_recv()
        total = summed[u, q].astype(jnp.float32)
        for r in range(1, GROUP):
            total = total + peers[u, r - 1].astype(jnp.float32)
        out[:, pl.ds(pl.multiple_of(u * COLS, COLS), COLS)] = total.astype(out.dtype)
        return carry

    lax.fori_loop(0, units // CORES, last, 0)

    def drain(u, carry):
        for r in range(1, GROUP):
            red(u, r).wait_send()
        for b in range(GROUP):
            part(u, b).wait_send()
        return carry

    lax.fori_loop(0, units // CORES, drain, 0)
    for kind in (0, 1):
        for r in range(1, GROUP):
            level(kind, r).wait_send()

        def drained(i, carry):
            each_way(kind, i // GROUP, i % GROUP, finish_send)
            return carry

        lax.fori_loop(0, layers * GROUP, drained, 0)
    for r in (1, 2):
        for s in (0, 1):
            hand(r, s).wait_send()
    pass_on(1, 2, 0).wait_send()
    pass_on(2, 1, 1).wait_send()
    for r in (1, 2, 3):
        for s in (0, 1):
            share(r, s).wait_send()


def grouped(layers, tokens, norm_gain, up_weight, up_scale, down_weight, down_scale):
    values = tokens.astype(jnp.float32)
    normed = (
        values * lax.rsqrt(jnp.mean(values * values, axis=-1, keepdims=True) + 1e-06) * norm_gain
    ).astype(jnp.bfloat16)
    up_cast = up_weight.astype(jnp.bfloat16)
    down_cast = down_weight.astype(jnp.bfloat16)
    rows, model = tokens.shape
    depth = up_weight.shape[0]
    width = up_weight.shape[1] // GROUP
    share = model // COLS // CORES
    n = layers * GROUP
    dma = pltpu.SemaphoreType.DMA
    vmem = pl.BlockSpec(memory_space=pltpu.VMEM)
    hbm = pl.BlockSpec(memory_space=pltpu.HBM)
    return pl.pallas_call(
        functools.partial(layer_kernel, layers, rows),
        out_shape=jax.ShapeDtypeStruct((rows, model // CORES), jnp.bfloat16),
        in_specs=[hbm, hbm, hbm, vmem, vmem],
        out_specs=vmem,
        scratch_shapes=[
            pltpu.VMEM((GROUP * rows, model), jnp.bfloat16),
            pltpu.VMEM((model, width), jnp.bfloat16),
            pltpu.VMEM((layers, width, GROUP * depth), jnp.bfloat16),
            pltpu.VMEM((GROUP * rows, width), jnp.bfloat16),
            pltpu.VMEM((share, GROUP, rows, COLS), jnp.bfloat16),
            pltpu.VMEM((share, GROUP, rows, COLS), jnp.bfloat16),
            pltpu.VMEM((share, GROUP, rows, COLS), jnp.bfloat16),
            pltpu.VMEM((share, GROUP - 1, rows, COLS), jnp.bfloat16),
            pltpu.VMEM((GROUP, rows, COLS), jnp.float32),
            dma((3,)),
            dma((2, n)),
            dma((2, n, 2)),
            dma((2, GROUP - 1)),
            dma((GROUP - 1, 2)),
            dma((GROUP - 1, 2)),
            dma((GROUP - 1, 2)),
            dma((GROUP - 1, 2)),
            dma((share, GROUP)),
            dma((share, GROUP)),
            dma((share, GROUP - 1)),
            dma((share, GROUP - 1)),
        ],
        compiler_params=pltpu.CompilerParams(
            collective_id=0, has_side_effects=True, vmem_limit_bytes=62 * 2**20
        ),
    )(normed, up_cast, down_cast, up_scale.reshape(1, -1), down_scale)


def solution(mesh):
    fs, tp = mesh.shape["fs"], mesh.shape["tp"]
    if tp == CORES and fs % (2 * GROUP) == 0 and fs <= 4 * GROUP:
        body = functools.partial(grouped, fs // GROUP)
    else:
        body = gathered
    in_specs = (P("fs", None), P(), P("fs", "tp"), P("tp"), P("tp", "fs"), P())
    out_specs = P("fs", "tp")
    return jax.shard_map(
        body, mesh=mesh, in_specs=in_specs, out_specs=out_specs, check_vma=False
    )
```

```python
import functools

import jax
import jax.numpy as jnp
from jax import lax
from jax.experimental import pallas as pl
from jax.experimental.pallas import tpu as pltpu
from jax.sharding import PartitionSpec as P

MESH = pl.DeviceIdType.MESH
SIDE = 2
GROUP = SIDE * SIDE
CORES = 2
COLS = 256
STRIP = 32


def gathered(tokens, norm_gain, up_weight, up_scale, down_weight, down_scale):
    values = tokens.astype(jnp.float32)
    normed = (
        values * lax.rsqrt(jnp.mean(values * values, axis=-1, keepdims=True) + 1e-06) * norm_gain
    ).astype(jnp.bfloat16)
    up_cast = up_weight.astype(jnp.bfloat16)
    down_cast = down_weight.astype(jnp.bfloat16)
    up_full = lax.all_gather(up_cast, "fs", axis=0, tiled=True)
    pre = jnp.dot(normed, up_full, preferred_element_type=jnp.float32) * up_scale
    hidden = jnp.square(jnp.maximum(pre, 0.0)).astype(jnp.bfloat16)
    down_full = lax.all_gather(down_cast, "fs", axis=1, tiled=True)
    partial_value = jnp.dot(hidden, down_full, preferred_element_type=jnp.float32) * down_scale
    rounded = partial_value.astype(jnp.bfloat16)
    return (
        lax.psum_scatter(rounded, "tp", scatter_dimension=1, tiled=True)
        .astype(jnp.float32)
        .astype(jnp.bfloat16)
    )


def layer_kernel(
    layers, rows, tokens, gain, up_in, down_in, up_scale, down_scale, out,
    tok, upb, downb, hid, stage, partner, summed, peers, own,
    local_sem, piece_recv, piece_send, level_send, tok_recv, tok_send,
    mate_recv, mate_send, part_recv, part_send, red_recv, red_send,
):
    fs = lax.axis_index("fs")
    core = lax.axis_index("tp")
    z, q = fs // GROUP, fs % GROUP
    depth, width = up_in.shape[0], upb.shape[1]
    half = rows // CORES
    sub = half // 2
    units = 2 * layers
    per_layer = GROUP * depth // COLS
    per_unit = COLS // depth

    def at(r):
        return ((q // SIDE + r // SIDE) % SIDE) * SIDE + (q % SIDE + r % SIDE) % SIDE

    def chip(layer, inner):
        return (layer * GROUP + inner, core)

    mate = (fs, 1 - core)

    barrier = pltpu.get_barrier_semaphore()
    for r in range(1, GROUP):
        pl.semaphore_signal(barrier, inc=1, device_id=chip(z, at(r)), device_id_type=MESH)
    pl.semaphore_signal(barrier, inc=1, device_id=mate, device_id_type=MESH)

    @pl.when(z > 0)
    def _():
        pl.semaphore_signal(barrier, inc=1, device_id=chip(z - 1, q), device_id_type=MESH)

    @pl.when(z < layers - 1)
    def _():
        pl.semaphore_signal(barrier, inc=1, device_id=chip(z + 1, q), device_id_type=MESH)

    def slot(kind, layer, inner):
        if kind == 0:
            return upb.at[pl.ds(pl.multiple_of((layer * GROUP + inner) * depth, depth), depth), :]
        return downb.at[layer, :, pl.ds(pl.multiple_of(inner * depth, depth), depth)]

    def source(kind, inner):
        if kind == 0:
            return up_in.at[:, pl.ds(pl.multiple_of(inner * width, width), width)]
        return down_in.at[pl.ds(pl.multiple_of(inner * width, width), width), :]

    def remote(src, dst, send, recv, device):
        return pltpu.make_async_remote_copy(
            src_ref=src, dst_ref=dst, send_sem=send, recv_sem=recv,
            device_id=device, device_id_type=MESH,
        )

    def along(kind, layer, inner, way):
        piece = slot(kind, layer, inner)
        index = layer * GROUP + inner
        return remote(
            piece, piece, piece_send.at[kind, index, way], piece_recv.at[kind, index],
            chip(z + 2 * way - 1, q),
        )

    def level(kind, r):
        return remote(
            source(kind, at(r)), slot(kind, z, q), level_send.at[kind, r - 1],
            piece_recv.at[kind, fs], chip(z, at(r)),
        )

    def each_way(kind, layer, inner, act):
        @pl.when(jnp.logical_and(layer <= z, z < layers - 1))
        def _():
            act(along(kind, layer, inner, 1))

        @pl.when(jnp.logical_and(layer >= z, z > 0))
        def _():
            act(along(kind, layer, inner, 0))

    def start(copy):
        copy.start()

    def finish_send(copy):
        copy.wait_send()

    def arrived(kind, layer, inner):
        piece = slot(kind, layer, inner)
        remote(
            piece, piece, piece_send.at[kind, layer * GROUP + inner, 0],
            piece_recv.at[kind, layer * GROUP + inner], mate,
        ).wait_recv()

    def block(inner, side, s):
        return tok.at[pl.ds(pl.multiple_of(inner * rows + side * half + s * sub, sub), sub), :]

    def hand(r, s):
        piece = block(q, core, s)
        return remote(piece, piece, tok_send.at[r - 1, s], tok_recv.at[r - 1, s], chip(z, at(r)))

    def pass_on(came, to, s):
        piece = block(at(came), core, s)
        return remote(
            piece, piece, tok_send.at[GROUP - 2, s], tok_recv.at[GROUP - 2, s], chip(z, at(to))
        )

    def tok_arrived(r, s):
        piece = block(at(r), core, s)
        remote(piece, piece, tok_send.at[r - 1, s], tok_recv.at[r - 1, s], mate).wait_recv()

    def share(r, s):
        piece = block(at(r), core, s)
        return remote(piece, piece, mate_send.at[r, s], mate_recv.at[r, s], mate)

    half_at = pl.ds(pl.multiple_of(q * rows + core * half, half), half)
    mine_at = pl.ds(pl.multiple_of(core * half, half), half)
    locals_ = [
        pltpu.make_async_copy(source(0, q), slot(0, z, q), local_sem.at[0]),
        pltpu.make_async_copy(source(1, q), slot(1, z, q), local_sem.at[1]),
        pltpu.make_async_copy(tokens.at[mine_at, :], tok.at[half_at, :], local_sem.at[2]),
    ]
    for copy in locals_:
        copy.start()
    greeted = GROUP + jnp.where(z > 0, 1, 0) + jnp.where(z < layers - 1, 1, 0)
    pl.semaphore_wait(barrier, greeted)

    for r in (3, 1, 2):
        level(0, r).start()
    for copy in locals_:
        copy.wait()
    each_way(0, z, q, start)

    def normalize(i, carry):
        strip = pl.ds(pl.multiple_of(q * rows + core * half + i * STRIP, STRIP), STRIP)
        values = tok[strip, :].astype(jnp.float32)
        mean = jnp.mean(values * values, axis=-1, keepdims=True)
        tok[strip, :] = (values * lax.rsqrt(mean + 1e-06) * gain[...]).astype(tok.dtype)
        return carry

    lax.fori_loop(0, half // STRIP, normalize, 0)
    hand(1, 0).start()
    hand(2, 1).start()
    hand(1, 1).start()
    hand(2, 0).start()
    for s in (0, 1):
        share(0, s).start()
    for r in (1, 2, 3):
        arrived(0, z, at(r))
        each_way(0, z, at(r), start)

    def from_afar(d):
        for r in range(GROUP):
            @pl.when(z - d >= 0)
            def _():
                arrived(0, z - d, at(r))
                each_way(0, z - d, at(r), start)

            @pl.when(z + d < layers)
            def _():
                arrived(0, z + d, at(r))
                each_way(0, z + d, at(r), start)

    for d in range(1, layers):
        from_afar(d)
        if d == 1:
            tok_arrived(1, 0)
            pass_on(1, 2, 0).start()
            share(1, 0).start()
            tok_arrived(2, 1)
            pass_on(2, 1, 1).start()
            share(2, 1).start()
            for r in (3, 1, 2):
                level(1, r).start()

    each_way(1, z, q, start)
    for r in (1, 2, 3):
        arrived(1, z, at(r))
        each_way(1, z, at(r), start)
    for r, s in ((1, 1), (2, 0), (3, 0), (3, 1)):
        tok_arrived(r, s)
        share(r, s).start()
    for r in (0, 1, 2, 3):
        for s in (0, 1):
            piece = block(at(r), 1 - core, s)
            remote(piece, piece, mate_send.at[r, s], mate_recv.at[r, s], mate).wait_recv()

    tall = rows * 2 // 3
    wide = 256
    across = width // wide

    def first(i, carry):
        m = pl.ds(pl.multiple_of((i // across) * tall, tall), tall)
        at_n = pl.multiple_of((i % across) * wide, wide)
        pre = jnp.dot(tok[m, :], upb[:, pl.ds(at_n, wide)], preferred_element_type=jnp.float32)
        pre = pre * up_scale[:, pl.ds(pl.multiple_of(q * width + at_n, wide), wide)]
        hid[m, pl.ds(at_n, wide)] = jnp.square(jnp.maximum(pre, 0.0)).astype(hid.dtype)
        return carry

    lax.fori_loop(0, (GROUP * rows // tall) * across, first, 0)

    upper, lower = pl.ds(0, half), pl.ds(half, half)
    hops = ((3, upper, 2, 1), (3, lower, 2, 2), (1, upper, 0, 1), (2, lower, 1, 2),
            (1, lower, 0, 1), (2, upper, 1, 2))

    def red(u, k):
        of, part_rows, into, to = hops[k]
        return remote(
            summed.at[u, at(of), part_rows, :], peers.at[u, into, part_rows, :],
            red_send.at[u, k], red_recv.at[u, k], chip(z, at(to)),
        )

    def relay(u):
        for k, of, part_rows, then in ((0, 2, upper, 5), (1, 1, lower, 4)):
            red(u, k).wait_recv()
            total = summed[u, at(of), part_rows, :].astype(jnp.float32)
            total = total + peers[u, 2, part_rows, :].astype(jnp.float32)
            summed[u, at(of), part_rows, :] = total.astype(summed.dtype)
            red(u, then).start()

    def unit_of(t):
        s, h = t // per_layer, t % per_layer
        layer = jnp.where(
            2 * z < layers,
            jnp.where(s <= z, z - s, s),
            jnp.where(s <= layers - 1 - z, z + s, layers - 1 - s),
        )
        unit = layer * per_layer + h
        return s, h, layer, unit, unit // (units // CORES), unit % (units // CORES)

    def part(u, b):
        return remote(
            stage.at[u, b], partner.at[u, b], part_send.at[u, b], part_recv.at[u, b], mate
        )

    def second(t, carry):
        s, h, layer, unit, owner, u = unit_of(t)

        @pl.when(s > 0)
        def _():
            for k in range(per_unit):
                arrived(1, layer, h * per_unit + k)
                each_way(1, layer, h * per_unit + k, start)

        cols = pl.ds(pl.multiple_of(h * COLS, COLS), COLS)
        scale = pl.ds(pl.multiple_of(unit * COLS, COLS), COLS)

        def product(b):
            m = pl.ds(pl.multiple_of(b * rows, rows), rows)
            value = jnp.dot(hid[m, :], downb[layer, :, cols], preferred_element_type=jnp.float32)
            return value * down_scale[:, scale]

        @pl.when(owner != core)
        def _():
            def away(i, c):
                b = at(GROUP - 1 - i)
                stage[u, b] = product(b).astype(stage.dtype)
                part(u, b).start()
                return c

            lax.fori_loop(0, GROUP, away, 0)

        @pl.when(owner == core)
        def _():
            def mine(i, c):
                own[at(GROUP - 1 - i)] = product(at(GROUP - 1 - i))
                return c

            lax.fori_loop(0, GROUP, mine, 0)
            for r in (3, 2, 1, 0):
                b = at(r)
                part(u, b).wait_recv()
                summed[u, b] = (own[b] + partner[u, b].astype(jnp.float32)).astype(summed.dtype)
                for k in {3: (0, 1), 1: (2,), 2: (3,), 0: ()}[r]:
                    red(u, k).start()

        before = unit_of(jnp.maximum(t - 1, 0))

        @pl.when(jnp.logical_and(t > 0, before[4] == core))
        def _():
            relay(before[5])

        return carry

    lax.fori_loop(0, units, second, 0)
    final = unit_of(units - 1)

    @pl.when(final[4] == core)
    def _():
        relay(final[5])

    def last(u, carry):
        for k in range(2, 6):
            red(u, k).wait_recv()
        total = summed[u, q].astype(jnp.float32)
        for side in range(2):
            total = total + peers[u, side].astype(jnp.float32)
        out[:, pl.ds(pl.multiple_of(u * COLS, COLS), COLS)] = total.astype(out.dtype)
        return carry

    lax.fori_loop(0, units // CORES, last, 0)

    def drain(u, carry):
        for k in range(len(hops)):
            red(u, k).wait_send()
        for b in range(GROUP):
            part(u, b).wait_send()
        return carry

    lax.fori_loop(0, units // CORES, drain, 0)
    for kind in (0, 1):
        for r in range(1, GROUP):
            level(kind, r).wait_send()

        def drained(i, carry):
            each_way(kind, i // GROUP, i % GROUP, finish_send)
            return carry

        lax.fori_loop(0, layers * GROUP, drained, 0)
    for r in (1, 2):
        for s in (0, 1):
            hand(r, s).wait_send()
    pass_on(1, 2, 0).wait_send()
    pass_on(2, 1, 1).wait_send()
    for r in (0, 1, 2, 3):
        for s in (0, 1):
            share(r, s).wait_send()


def grouped(layers, tokens, norm_gain, up_weight, up_scale, down_weight, down_scale):
    up_cast = up_weight.astype(jnp.bfloat16)
    down_cast = down_weight.astype(jnp.bfloat16)
    rows, model = tokens.shape
    depth = up_weight.shape[0]
    width = up_weight.shape[1] // GROUP
    share = model // COLS // CORES
    n = layers * GROUP
    dma = pltpu.SemaphoreType.DMA
    vmem = pl.BlockSpec(memory_space=pltpu.VMEM)
    hbm = pl.BlockSpec(memory_space=pltpu.HBM)
    return pl.pallas_call(
        functools.partial(layer_kernel, layers, rows),
        out_shape=jax.ShapeDtypeStruct((rows, model // CORES), jnp.bfloat16),
        in_specs=[hbm, vmem, hbm, hbm, vmem, vmem],
        out_specs=vmem,
        scratch_shapes=[
            pltpu.VMEM((GROUP * rows, model), jnp.bfloat16),
            pltpu.VMEM((model, width), jnp.bfloat16),
            pltpu.VMEM((layers, width, GROUP * depth), jnp.bfloat16),
            pltpu.VMEM((GROUP * rows, width), jnp.bfloat16),
            pltpu.VMEM((share, GROUP, rows, COLS), jnp.bfloat16),
            pltpu.VMEM((share, GROUP, rows, COLS), jnp.bfloat16),
            pltpu.VMEM((share, GROUP, rows, COLS), jnp.bfloat16),
            pltpu.VMEM((share, GROUP - 1, rows, COLS), jnp.bfloat16),
            pltpu.VMEM((GROUP, rows, COLS), jnp.float32),
            dma((3,)),
            dma((2, n)),
            dma((2, n, 2)),
            dma((2, GROUP - 1)),
            dma((GROUP - 1, 2)),
            dma((GROUP - 1, 2)),
            dma((GROUP, 2)),
            dma((GROUP, 2)),
            dma((share, GROUP)),
            dma((share, GROUP)),
            dma((share, 6)),
            dma((share, 6)),
        ],
        compiler_params=pltpu.CompilerParams(
            collective_id=0, has_side_effects=True, vmem_limit_bytes=62 * 2**20
        ),
    )(tokens, norm_gain.reshape(1, -1), up_cast, down_cast, up_scale.reshape(1, -1), down_scale)


def solution(mesh):
    fs, tp = mesh.shape["fs"], mesh.shape["tp"]
    if tp == CORES and fs % (2 * GROUP) == 0 and fs <= 4 * GROUP:
        body = functools.partial(grouped, fs // GROUP)
    else:
        body = gathered
    in_specs = (P("fs", None), P(), P("fs", "tp"), P("tp"), P("tp", "fs"), P())
    out_specs = P("fs", "tp")
    return jax.shard_map(
        body, mesh=mesh, in_specs=in_specs, out_specs=out_specs, check_vma=False
    )
```

```python
import functools

import jax
import jax.numpy as jnp
from jax import lax
from jax.experimental import pallas as pl
from jax.experimental.pallas import tpu as pltpu
from jax.sharding import PartitionSpec as P

MESH = pl.DeviceIdType.MESH
SIDE = 2
GROUP = SIDE * SIDE
CORES = 2
COLS = 256
STRIP = 32


def gathered(tokens, norm_gain, up_weight, up_scale, down_weight, down_scale):
    values = tokens.astype(jnp.float32)
    normed = (
        values * lax.rsqrt(jnp.mean(values * values, axis=-1, keepdims=True) + 1e-06) * norm_gain
    ).astype(jnp.bfloat16)
    up_cast = up_weight.astype(jnp.bfloat16)
    down_cast = down_weight.astype(jnp.bfloat16)
    up_full = lax.all_gather(up_cast, "fs", axis=0, tiled=True)
    pre = jnp.dot(normed, up_full, preferred_element_type=jnp.float32) * up_scale
    hidden = jnp.square(jnp.maximum(pre, 0.0)).astype(jnp.bfloat16)
    down_full = lax.all_gather(down_cast, "fs", axis=1, tiled=True)
    partial_value = jnp.dot(hidden, down_full, preferred_element_type=jnp.float32) * down_scale
    rounded = partial_value.astype(jnp.bfloat16)
    return (
        lax.psum_scatter(rounded, "tp", scatter_dimension=1, tiled=True)
        .astype(jnp.float32)
        .astype(jnp.bfloat16)
    )


def layer_kernel(
    layers, rows, tokens, gain, up_in, down_in, up_scale, down_scale, out,
    tok, upb, downb, hid, stage, partner, summed, peers, own,
    local_sem, piece_recv, piece_send, level_send, tok_recv, tok_send,
    mate_recv, mate_send, part_recv, part_send, red_recv, red_send,
):
    fs = lax.axis_index("fs")
    core = lax.axis_index("tp")
    z, q = fs // GROUP, fs % GROUP
    depth, width = up_in.shape[0], upb.shape[1]
    half = rows // CORES
    sub = half // 2
    units = 2 * layers
    per_layer = GROUP * depth // COLS
    per_unit = COLS // depth

    def at(r):
        return ((q // SIDE + r // SIDE) % SIDE) * SIDE + (q % SIDE + r % SIDE) % SIDE

    def chip(layer, inner):
        return (layer * GROUP + inner, core)

    mate = (fs, 1 - core)

    barrier = pltpu.get_barrier_semaphore()
    for r in range(1, GROUP):
        pl.semaphore_signal(barrier, inc=1, device_id=chip(z, at(r)), device_id_type=MESH)
    pl.semaphore_signal(barrier, inc=1, device_id=mate, device_id_type=MESH)

    @pl.when(z > 0)
    def _():
        pl.semaphore_signal(barrier, inc=1, device_id=chip(z - 1, q), device_id_type=MESH)

    @pl.when(z < layers - 1)
    def _():
        pl.semaphore_signal(barrier, inc=1, device_id=chip(z + 1, q), device_id_type=MESH)

    def slot(kind, layer, inner):
        if kind == 0:
            return upb.at[pl.ds(pl.multiple_of((layer * GROUP + inner) * depth, depth), depth), :]
        return downb.at[layer, :, pl.ds(pl.multiple_of(inner * depth, depth), depth)]

    def source(kind, inner):
        if kind == 0:
            return up_in.at[:, pl.ds(pl.multiple_of(inner * width, width), width)]
        return down_in.at[pl.ds(pl.multiple_of(inner * width, width), width), :]

    def remote(src, dst, send, recv, device):
        return pltpu.make_async_remote_copy(
            src_ref=src, dst_ref=dst, send_sem=send, recv_sem=recv,
            device_id=device, device_id_type=MESH,
        )

    def along(kind, layer, inner, way):
        piece = slot(kind, layer, inner)
        index = layer * GROUP + inner
        return remote(
            piece, piece, piece_send.at[kind, index, way], piece_recv.at[kind, index],
            chip(z + 2 * way - 1, q),
        )

    def level(kind, r):
        return remote(
            source(kind, at(r)), slot(kind, z, q), level_send.at[kind, r - 1],
            piece_recv.at[kind, fs], chip(z, at(r)),
        )

    def each_way(kind, layer, inner, act):
        @pl.when(jnp.logical_and(layer <= z, z < layers - 1))
        def _():
            act(along(kind, layer, inner, 1))

        @pl.when(jnp.logical_and(layer >= z, z > 0))
        def _():
            act(along(kind, layer, inner, 0))

    def start(copy):
        copy.start()

    def finish_send(copy):
        copy.wait_send()

    def arrived(kind, layer, inner):
        piece = slot(kind, layer, inner)
        remote(
            piece, piece, piece_send.at[kind, layer * GROUP + inner, 0],
            piece_recv.at[kind, layer * GROUP + inner], mate,
        ).wait_recv()

    def block(inner, side, s):
        return tok.at[pl.ds(pl.multiple_of(inner * rows + side * half + s * sub, sub), sub), :]

    def hand(r, s):
        piece = block(q, core, s)
        return remote(piece, piece, tok_send.at[r - 1, s], tok_recv.at[r - 1, s], chip(z, at(r)))

    def pass_on(came, to, s):
        piece = block(at(came), core, s)
        return remote(
            piece, piece, tok_send.at[GROUP - 2, s], tok_recv.at[GROUP - 2, s], chip(z, at(to))
        )

    def tok_arrived(r, s):
        piece = block(at(r), core, s)
        remote(piece, piece, tok_send.at[r - 1, s], tok_recv.at[r - 1, s], mate).wait_recv()

    def share(r, s):
        piece = block(at(r), core, s)
        return remote(piece, piece, mate_send.at[r, s], mate_recv.at[r, s], mate)

    half_at = pl.ds(pl.multiple_of(q * rows + core * half, half), half)
    mine_at = pl.ds(pl.multiple_of(core * half, half), half)
    locals_ = [
        pltpu.make_async_copy(source(0, q), slot(0, z, q), local_sem.at[0]),
        pltpu.make_async_copy(source(1, q), slot(1, z, q), local_sem.at[1]),
        pltpu.make_async_copy(tokens.at[mine_at, :], tok.at[half_at, :], local_sem.at[2]),
    ]
    for copy in locals_:
        copy.start()
    greeted = GROUP + jnp.where(z > 0, 1, 0) + jnp.where(z < layers - 1, 1, 0)
    pl.semaphore_wait(barrier, greeted)

    for r in (3, 1, 2):
        level(0, r).start()
    for copy in locals_:
        copy.wait()
    each_way(0, z, q, start)

    def normalize(i, carry):
        strip = pl.ds(pl.multiple_of(q * rows + core * half + i * STRIP, STRIP), STRIP)
        values = tok[strip, :].astype(jnp.float32)
        mean = jnp.mean(values * values, axis=-1, keepdims=True)
        tok[strip, :] = (values * lax.rsqrt(mean + 1e-06) * gain[...]).astype(tok.dtype)
        return carry

    lax.fori_loop(0, half // STRIP, normalize, 0)
    hand(1, 0).start()
    hand(2, 1).start()
    hand(1, 1).start()
    hand(2, 0).start()
    for r in (3, 1, 2):
        level(1, r).start()
    for s in (0, 1):
        share(0, s).start()
    for r in (1, 2, 3):
        arrived(0, z, at(r))
        each_way(0, z, at(r), start)

    def from_afar(d):
        for r in range(GROUP):
            @pl.when(z - d >= 0)
            def _():
                arrived(0, z - d, at(r))
                each_way(0, z - d, at(r), start)

            @pl.when(z + d < layers)
            def _():
                arrived(0, z + d, at(r))
                each_way(0, z + d, at(r), start)

    for d in range(1, layers):
        from_afar(d)
        if d == 1:
            tok_arrived(1, 0)
            pass_on(1, 2, 0).start()
            share(1, 0).start()
            tok_arrived(2, 1)
            pass_on(2, 1, 1).start()
            share(2, 1).start()
            for r in (1, 2, 3):
                arrived(1, z, at(r))
        for way, ahead in ((1, z), (0, layers - 1 - z)):
            due = ahead <= 1 if d == 1 else ahead == d

            @pl.when(jnp.logical_and(due, (layers - 1 - z if way else z) > 0))
            def _():
                for r in range(GROUP):
                    along(1, z, at(r), way).start()

    for r, s in ((1, 1), (2, 0), (3, 0), (3, 1)):
        tok_arrived(r, s)
        share(r, s).start()
    for r in (0, 1, 2, 3):
        for s in (0, 1):
            piece = block(at(r), 1 - core, s)
            remote(piece, piece, mate_send.at[r, s], mate_recv.at[r, s], mate).wait_recv()

    tall = rows * 2 // 3
    wide = 256
    across = width // wide

    def first(i, carry):
        m = pl.ds(pl.multiple_of((i // across) * tall, tall), tall)
        at_n = pl.multiple_of((i % across) * wide, wide)
        pre = jnp.dot(tok[m, :], upb[:, pl.ds(at_n, wide)], preferred_element_type=jnp.float32)
        pre = pre * up_scale[:, pl.ds(pl.multiple_of(q * width + at_n, wide), wide)]
        hid[m, pl.ds(at_n, wide)] = jnp.square(jnp.maximum(pre, 0.0)).astype(hid.dtype)
        return carry

    def take(d, r):
        for layer, there in ((z - d, z - d >= 0), (z + d, z + d < layers)):
            @pl.when(there)
            def _():
                arrived(1, layer, r)
                each_way(1, layer, r, start)

    inside = jnp.logical_and(z > 0, z < layers - 1)
    tiles = (GROUP * rows // tall) * across
    lax.fori_loop(0, tiles // 2, first, 0)

    @pl.when(inside)
    def _():
        for r in range(GROUP):
            take(1, r)

    lax.fori_loop(tiles // 2, tiles, first, 0)

    upper, lower = pl.ds(0, half), pl.ds(half, half)
    hops = ((3, upper, 2, 1), (3, lower, 2, 2), (1, upper, 0, 1), (2, lower, 1, 2),
            (1, lower, 0, 1), (2, upper, 1, 2))

    def red(u, k):
        of, part_rows, into, to = hops[k]
        return remote(
            summed.at[u, at(of), part_rows, :], peers.at[u, into, part_rows, :],
            red_send.at[u, k], red_recv.at[u, k], chip(z, at(to)),
        )

    def relay(u):
        for k, of, part_rows, then in ((0, 2, upper, 5), (1, 1, lower, 4)):
            red(u, k).wait_recv()
            total = summed[u, at(of), part_rows, :].astype(jnp.float32)
            total = total + peers[u, 2, part_rows, :].astype(jnp.float32)
            summed[u, at(of), part_rows, :] = total.astype(summed.dtype)
            red(u, then).start()

    def unit_of(t):
        s, h = t // per_layer, t % per_layer
        layer = jnp.where(
            2 * z < layers,
            jnp.where(s <= z, z - s, s),
            jnp.where(s <= layers - 1 - z, z + s, layers - 1 - s),
        )
        unit = layer * per_layer + h
        return s, h, layer, unit, unit // (units // CORES), unit % (units // CORES)

    def part(u, b):
        return remote(
            stage.at[u, b], partner.at[u, b], part_send.at[u, b], part_recv.at[u, b], mate
        )

    def second(t, carry):
        s, h, layer, unit, owner, u = unit_of(t)

        d = s + jnp.where(inside, 1, 0)

        @pl.when(d > jnp.where(inside, 1, 0))
        def _():
            for k in range(per_unit):
                take(d, h * per_unit + k)

        cols = pl.ds(pl.multiple_of(h * COLS, COLS), COLS)
        scale = pl.ds(pl.multiple_of(unit * COLS, COLS), COLS)

        def product(b):
            m = pl.ds(pl.multiple_of(b * rows, rows), rows)
            value = jnp.dot(hid[m, :], downb[layer, :, cols], preferred_element_type=jnp.float32)
            return value * down_scale[:, scale]

        @pl.when(owner != core)
        def _():
            def away(i, c):
                b = at(GROUP - 1 - i)
                stage[u, b] = product(b).astype(stage.dtype)
                part(u, b).start()
                return c

            lax.fori_loop(0, GROUP, away, 0)

        @pl.when(owner == core)
        def _():
            def mine(i, c):
                own[at(GROUP - 1 - i)] = product(at(GROUP - 1 - i))
                return c

            lax.fori_loop(0, GROUP, mine, 0)
            for r in (3, 2, 1, 0):
                b = at(r)
                part(u, b).wait_recv()
                summed[u, b] = (own[b] + partner[u, b].astype(jnp.float32)).astype(summed.dtype)
                for k in {3: (0, 1), 1: (2,), 2: (3,), 0: ()}[r]:
                    red(u, k).start()

        before = unit_of(jnp.maximum(t - 1, 0))

        @pl.when(jnp.logical_and(t > 0, before[4] == core))
        def _():
            relay(before[5])

        return carry

    lax.fori_loop(0, units, second, 0)
    final = unit_of(units - 1)

    @pl.when(final[4] == core)
    def _():
        relay(final[5])

    def last(u, carry):
        for k in range(2, 6):
            red(u, k).wait_recv()
        total = summed[u, q].astype(jnp.float32)
        for side in range(2):
            total = total + peers[u, side].astype(jnp.float32)
        out[:, pl.ds(pl.multiple_of(u * COLS, COLS), COLS)] = total.astype(out.dtype)
        return carry

    lax.fori_loop(0, units // CORES, last, 0)

    def drain(u, carry):
        for k in range(len(hops)):
            red(u, k).wait_send()
        for b in range(GROUP):
            part(u, b).wait_send()
        return carry

    lax.fori_loop(0, units // CORES, drain, 0)
    for kind in (0, 1):
        for r in range(1, GROUP):
            level(kind, r).wait_send()

        def drained(i, carry):
            each_way(kind, i // GROUP, i % GROUP, finish_send)
            return carry

        lax.fori_loop(0, layers * GROUP, drained, 0)
    for r in (1, 2):
        for s in (0, 1):
            hand(r, s).wait_send()
    pass_on(1, 2, 0).wait_send()
    pass_on(2, 1, 1).wait_send()
    for r in (0, 1, 2, 3):
        for s in (0, 1):
            share(r, s).wait_send()


def grouped(layers, tokens, norm_gain, up_weight, up_scale, down_weight, down_scale):
    up_cast = up_weight.astype(jnp.bfloat16)
    down_cast = down_weight.astype(jnp.bfloat16)
    rows, model = tokens.shape
    depth = up_weight.shape[0]
    width = up_weight.shape[1] // GROUP
    share = model // COLS // CORES
    n = layers * GROUP
    dma = pltpu.SemaphoreType.DMA
    vmem = pl.BlockSpec(memory_space=pltpu.VMEM)
    hbm = pl.BlockSpec(memory_space=pltpu.HBM)
    return pl.pallas_call(
        functools.partial(layer_kernel, layers, rows),
        out_shape=jax.ShapeDtypeStruct((rows, model // CORES), jnp.bfloat16),
        in_specs=[hbm, vmem, hbm, hbm, vmem, vmem],
        out_specs=vmem,
        scratch_shapes=[
            pltpu.VMEM((GROUP * rows, model), jnp.bfloat16),
            pltpu.VMEM((model, width), jnp.bfloat16),
            pltpu.VMEM((layers, width, GROUP * depth), jnp.bfloat16),
            pltpu.VMEM((GROUP * rows, width), jnp.bfloat16),
            pltpu.VMEM((share, GROUP, rows, COLS), jnp.bfloat16),
            pltpu.VMEM((share, GROUP, rows, COLS), jnp.bfloat16),
            pltpu.VMEM((share, GROUP, rows, COLS), jnp.bfloat16),
            pltpu.VMEM((share, GROUP - 1, rows, COLS), jnp.bfloat16),
            pltpu.VMEM((GROUP, rows, COLS), jnp.float32),
            dma((3,)),
            dma((2, n)),
            dma((2, n, 2)),
            dma((2, GROUP - 1)),
            dma((GROUP - 1, 2)),
            dma((GROUP - 1, 2)),
            dma((GROUP, 2)),
            dma((GROUP, 2)),
            dma((share, GROUP)),
            dma((share, GROUP)),
            dma((share, 6)),
            dma((share, 6)),
        ],
        compiler_params=pltpu.CompilerParams(
            collective_id=0, has_side_effects=True, vmem_limit_bytes=62 * 2**20
        ),
    )(tokens, norm_gain.reshape(1, -1), up_cast, down_cast, up_scale.reshape(1, -1), down_scale)


def solution(mesh):
    fs, tp = mesh.shape["fs"], mesh.shape["tp"]
    if tp == CORES and fs % (2 * GROUP) == 0 and fs <= 4 * GROUP:
        body = functools.partial(grouped, fs // GROUP)
    else:
        body = gathered
    in_specs = (P("fs", None), P(), P("fs", "tp"), P("tp"), P("tp", "fs"), P())
    out_specs = P("fs", "tp")
    return jax.shard_map(
        body, mesh=mesh, in_specs=in_specs, out_specs=out_specs, check_vma=False
    )
```
